32 devices in a mesh: ep: 4 (over y, x), tp: 8 (over z, core).
Axes of the slice: x: 2, y: 2, z: 4, core: 2. Of those that a mesh axis runs over, the one named last changes fastest.
Arguments:
- mix_tokens: bfloat16 [2048, 1, 1024], P(('ep', 'tp')), may hold values from -6 to 6
- mix_gain: float32 [1024], replicated, may hold values from 0.1 to 1.9
- w_query: bfloat16 [1024, 1024], replicated, may hold values from -0.1875 to 0.1875
- w_key: bfloat16 [1024, 256], replicated, may hold values from -0.1875 to 0.1875
- w_value: bfloat16 [1024, 256], replicated, may hold values from -0.1875 to 0.1875
- query_gain: float32 [64], replicated, may hold values from 1.2 to 14
- key_gain: float32 [64], replicated, may hold values from 1.2 to 14
- w_out: bfloat16 [1024, 1024], replicated, may hold values from -0.1875 to 0.1875
- expert_tokens: bfloat16 [4096, 1024], P(('ep', 'tp')), may hold values from -6 to 6
- expert_gain: float32 [1024], replicated, may hold values from 0.1 to 1.9
- route_ids: int32 [4096, 2], P(('ep', 'tp')), may hold values from 0 to 7, all different within a row; in each aligned block of 128 rows (0 to 127, 128 to 255, ...) at most 36 rows name the same one
- route_weights: float32 [4096, 2], P(('ep', 'tp')), may hold values from 0.1 to 1
- w_gate: bfloat16 [8, 1024, 4096], P('ep', None, 'tp'), may hold values from -0.1875 to 0.1875
- w_up: bfloat16 [8, 1024, 4096], P('ep', None, 'tp'), may hold values from -0.1875 to 0.1875
- w_down: bfloat16 [8, 4096, 1024], P('ep', 'tp'), may hold values from -0.09375 to 0.09375
Outputs:
- mix_out: bfloat16 [2048, 1, 1024], P(('ep', 'tp'))
- experts_out: bfloat16 [4096, 1024], P(('ep', 'tp'))
The draws below stay inside these ranges and needn't reach their ends.
Inputs may be any that keep to these rules, and one draw needn't show every extreme that they name: `route_ids`: each row names 2 different experts. Among the rows of one device no expert is named more than 36 times, and in every draw some expert is named exactly 36 times by the rows of some device.
All inputs are finite; a program needn't handle non-finite values.
Results may differ from the reference program's by a relative error of at most 0.018.
The reference program's roundings to bfloat16 on the way count: a program that leaves them out, or rounds other values in their place, can miss the bound.
Values may be sent and summed in bfloat16 or wider, within the bound.
No kernel may reach another device: no remote copies, remote signals or barrier semaphores. Data moves between devices by JAX's collectives and lax.ppermute only.
A program may use at most 128 MiB of HBM per device.

```python
import math
import jax
import jax.numpy as jnp
import numpy as np
from jax import lax

D = 1024
HEADS = 16
KV_HEADS = 4
HEAD = 64
GRID_W = 64
FF = 4096
EXPERTS = 8
TOP_K = 2
SEQS = 1
LEN = 2048
TOK_EXP = 128
TOKENS = 4096
CAP = 36
N_TP = 8


def draw_gain_pair(base_key):
    base_gain = jax.random.uniform(jax.random.fold_in(base_key, 1), (HEAD,), jnp.float32, 1.2, 2.2)
    return base_gain


def draw_query_gain(key, part):
    return draw_gain_pair(jax.random.fold_in(key, 17))


def draw_key_gain(key, part):
    return draw_gain_pair(jax.random.fold_in(key, 29))


def shard_levels(own_key, dims, split, least, largest):
    loudness, own = 1.0, jax.random.fold_in(own_key, 6)
    for dim, shards_of in split:
        draws = jnp.exp(jax.random.uniform(jax.random.fold_in(own, dim), (shards_of,), jnp.float32, least / len(split), largest / len(split)))
        loudness = loudness * jnp.repeat(draws, dims[dim] // shards_of).reshape([-1 if axis == dim else 1 for axis in range(len(dims))])
    return loudness


def assign_block(own_key, own, number, rows, number_of, top, most, skew):
    sequence = jax.random.permutation(own_key, number_of)
    crowded, usual = load_shares(number_of, rows * top, most, skew, True), load_shares(number_of, rows * top, most, skew, False)
    places = jnp.arange(number_of)

    def named(sizes, offset_by):
        used = int((sizes > 0).sum())
        fixed = max(1, used // 4)
        shifted = fixed + (places - fixed + offset_by * (used - fixed)) % max(1, number_of - fixed)
        return jnp.zeros((number_of,), jnp.int32).at[sequence[jnp.where(places < fixed, places, shifted)]].set(jnp.asarray(sizes, jnp.int32))

    sizes = jnp.where(number % 4 == 0, named(crowded, number // 4), named(usual, number - number // 4 - 1))
    mixed = jax.random.permutation(jax.random.fold_in(own, 3), number_of)
    source_of, sink = mixed[0:number_of // 2 * 2:2], mixed[1:number_of // 2 * 2:2]
    room = jnp.minimum(sizes[source_of] - 1, most - sizes[sink]) // 2
    room = jnp.where((source_of == sequence[0]) | (sink == sequence[0]) | (sizes[sink] == 0), 0, jnp.maximum(room, 0))
    shifted = jax.random.randint(jax.random.fold_in(own, 4), (number_of // 2,), 0, 1 << 20) % (room + 1)
    sizes = sizes.at[source_of].add(-shifted).at[sink].add(shifted)
    members = jnp.searchsorted(jnp.cumsum(sizes), jnp.arange(rows * top), side="right").astype(jnp.int32)
    grid = members.reshape(top, rows).T
    grid = grid[jax.random.permutation(jax.random.fold_in(own, 1), rows)]
    offset_by = jax.random.randint(jax.random.fold_in(own, 2), (rows, 1), 0, top)
    return jnp.take_along_axis(grid, (jnp.arange(top)[None, :] + offset_by) % top, axis=1)


def load_shares(amount, total, most, skew, full):
    weights = [(1 << 20) // math.isqrt(standing ** skew) + 1 for standing in range(1, amount + 1)]
    largest = most if full else min(most, max(-(-total // amount), total * weights[0] // sum(weights)))
    least = 1 if total - largest >= amount - 1 else 0
    counts, spare = [largest] + [least] * (amount - 1), total - largest - least * (amount - 1)
    while spare > 0:
        free = [i for i in range(1, amount) if counts[i] < largest] or [i for i in range(1, amount) if counts[i] < most]
        mass, budget = sum([weights[i] for i in free]), spare
        for i in free:
            extra = min(most - counts[i], max(1, budget * weights[i] // mass), spare)
            counts[i] = counts[i] + extra
            spare = spare - extra
    return np.array(counts)


def centred(stream_key, extent, scale, limit, pieces=(), kind=jnp.bfloat16):
    factor_of = shard_levels(stream_key, extent, pieces, -0.22, 0.18) if pieces else 1.0
    values = jax.random.normal(stream_key, extent, jnp.float32) * scale * factor_of
    return jnp.minimum(jnp.maximum(values, -limit), limit).astype(kind)


def setup_inputs(seed: int = 0) -> dict:
    key_list = jax.random.split(jax.random.key(seed), 16)
    mix_tokens = centred(key_list[0], (LEN, SEQS, D), 1.0, 6.0, ((0, 32),))
    mix_gain = jnp.clip(1.0 + 0.18 * jax.random.normal(key_list[1], (D,), jnp.float32), 0.1, 1.9)
    w_query = centred(key_list[2], (D, HEADS * HEAD), D ** -0.5, 0.1875)
    w_key = centred(key_list[3], (D, KV_HEADS * HEAD), D ** -0.5, 0.1875)
    w_value = centred(key_list[4], (D, KV_HEADS * HEAD), D ** -0.5, 0.1875)
    query_gain = draw_query_gain(jax.random.fold_in(key_list[15], 71), 0)
    key_gain = draw_key_gain(jax.random.fold_in(key_list[15], 71), 0)
    w_out = centred(key_list[7], (HEADS * HEAD, D), (HEADS * HEAD) ** -0.5, 0.1875)
    expert_tokens = centred(key_list[8], (TOKENS, D), 1.0, 6.0, ((0, 32),))
    expert_gain = jnp.clip(1.0 + 0.18 * jax.random.normal(key_list[9], (D,), jnp.float32), 0.1, 1.9)
    route_ids_keys = jax.random.split(jax.random.fold_in(key_list[10], 1), TOKENS // TOK_EXP)
    route_ids_turns = jax.random.permutation(jax.random.fold_in(key_list[10], 3), TOKENS // TOK_EXP)
    route_ids = jax.vmap(lambda own, number: assign_block(jax.random.fold_in(key_list[10], 2), own, number, TOK_EXP, EXPERTS, TOP_K, CAP, 1))(route_ids_keys, route_ids_turns).reshape((TOKENS, TOP_K))
    route_weights = jnp.clip(jnp.exp(math.log(1.0) - 2.3025851 * jax.random.uniform(key_list[11], (TOKENS, TOP_K), jnp.float32) ** shard_levels(key_list[11], (TOKENS, TOP_K), ((0, 32),), -0.2, 0.2)), 0.1, 1.0)
    w_gate = centred(key_list[12], (EXPERTS, D, FF), D ** -0.5, 0.1875, ((0, 4), (2, 8)))
    w_up = centred(key_list[13], (EXPERTS, D, FF), D ** -0.5, 0.1875, ((0, 4), (2, 8)))
    w_down = centred(key_list[14], (EXPERTS, FF, D), FF ** -0.5, 0.09375, ((0, 4), (1, 8)))
    return dict(mix_tokens=mix_tokens, mix_gain=mix_gain, w_query=w_query, w_key=w_key, w_value=w_value, query_gain=query_gain, key_gain=key_gain, w_out=w_out, expert_tokens=expert_tokens, expert_gain=expert_gain, route_ids=route_ids, route_weights=route_weights, w_gate=w_gate, w_up=w_up, w_down=w_down)


epsilon = 1e-06

def normalize(values, gain_vec):
    widened = values.astype(jnp.float32)
    return widened * lax.rsqrt(lax.optimization_barrier(jnp.mean(widened * widened, axis=-1, keepdims=True)) + epsilon) * gain_vec

def angle_tables(positions, head_size):
    quarter = head_size // 4
    frequency = 10000.0 ** (-jnp.arange(quarter, dtype=jnp.float32) / quarter)
    grid_pos = jnp.stack([positions // GRID_W, positions % GRID_W], axis=-1).astype(jnp.float32)
    angles = grid_pos[:, :, None] * frequency[None, None, :]
    return (jnp.cos(angles), jnp.sin(angles))

def turn(values, cosine_table, sine_table):
    shaped = values.shape
    quarter = shaped[-1] // 4
    leading = (shaped[0],) + (1,) * (len(shaped) - 2) + (2, quarter)
    cosine_table = cosine_table.reshape(leading)
    sine_table = sine_table.reshape(leading)
    halves = values.reshape(shaped[:-1] + (2, 2, quarter))
    first_part = halves[..., 0, :]
    second_part = halves[..., 1, :]
    turned = jnp.stack([first_part * cosine_table - second_part * sine_table, first_part * sine_table + second_part * cosine_table], axis=-2)
    return turned.reshape(shaped)

def mixer_reference(mix_tokens, mix_gain, w_query, w_key, w_value, query_gain, key_gain, w_out):
    normed = normalize(mix_tokens, mix_gain).astype(jnp.bfloat16)
    queries = jnp.dot(normed, w_query, preferred_element_type=jnp.float32).astype(jnp.bfloat16)
    keys_raw = jnp.dot(normed, w_key, preferred_element_type=jnp.float32).astype(jnp.bfloat16)
    values = jnp.dot(normed, w_value, preferred_element_type=jnp.float32).astype(jnp.bfloat16)
    group_size = HEADS // KV_HEADS
    cosine_table, sine_table = angle_tables(jnp.arange(LEN, dtype=jnp.int32), HEAD)
    query_heads = normalize(queries.reshape(LEN, SEQS, HEADS, HEAD), query_gain)
    turned_queries = turn(query_heads, cosine_table, sine_table).astype(jnp.bfloat16)
    turned_queries = turned_queries.reshape(LEN, SEQS, KV_HEADS, group_size, HEAD)
    key_heads = normalize(keys_raw.reshape(LEN, SEQS, KV_HEADS, HEAD), key_gain)
    turned_keys = turn(key_heads, cosine_table, sine_table).astype(jnp.bfloat16).astype(jnp.float32)
    value_heads = values.reshape(LEN, SEQS, KV_HEADS, HEAD).astype(jnp.float32)
    block_rows = math.gcd(LEN, 128)

    def attend(query_block):
        scores = jnp.einsum('qskgd,lskd->qskgl', query_block.astype(jnp.float32), turned_keys) * HEAD ** (-0.5)
        row_max = lax.optimization_barrier(jnp.max(scores, axis=-1, keepdims=True))
        raised = jnp.exp(scores - row_max)
        totals = lax.optimization_barrier(jnp.sum(raised, axis=-1))
        weights = lax.optimization_barrier(raised.astype(jnp.bfloat16)).astype(jnp.float32)
        mixed = jnp.einsum('qskgl,lskd->qskgd', weights, value_heads) / totals[..., None]
        return mixed.astype(jnp.bfloat16)
    blocks = turned_queries.reshape(LEN // block_rows, block_rows, SEQS, KV_HEADS, group_size, HEAD)
    outputs = lax.map(attend, blocks)
    mixed_heads = outputs.reshape(LEN, SEQS, HEADS * HEAD)
    return jnp.dot(mixed_heads, w_out, preferred_element_type=jnp.float32).astype(jnp.bfloat16)

def experts_reference(expert_tokens, expert_gain, route_ids, route_weights, w_gate, w_up, w_down):
    tok_total = expert_tokens.shape[0]
    block_count = tok_total // TOK_EXP
    normed = normalize(expert_tokens, expert_gain).astype(jnp.bfloat16)
    grouped = route_ids.reshape(block_count, TOK_EXP * TOP_K)
    matches = (grouped[:, :, None] == jnp.arange(EXPERTS, dtype=jnp.int32)[None, None, :]).astype(jnp.int32)
    rank_ids = lax.optimization_barrier(jnp.sum((jnp.cumsum(matches, axis=1) - 1) * matches, axis=2)).astype(jnp.int32)
    slot_ids = (jnp.arange(block_count, dtype=jnp.int32)[:, None] * CAP + rank_ids).reshape(-1).astype(jnp.int32)
    flat_ids = grouped.reshape(-1).astype(jnp.int32)
    token_ids = (jnp.arange(tok_total * TOP_K, dtype=jnp.int32) // TOP_K).astype(jnp.int32)
    buffer_rows = jnp.zeros((EXPERTS, block_count * CAP, D), jnp.bfloat16).at[flat_ids, slot_ids].set(normed[token_ids])

    def run_expert(operands):
        rows_in, gate_w, up_w, down_w = operands
        gate_act = jnp.dot(rows_in, gate_w, preferred_element_type=jnp.float32)
        up_act = jnp.dot(rows_in, up_w, preferred_element_type=jnp.float32)
        hidden = (jax.nn.silu(gate_act) * up_act).astype(jnp.bfloat16)
        hidden_groups = hidden.reshape(-1, N_TP, FF // N_TP).astype(jnp.float32)
        down_groups = down_w.reshape(N_TP, FF // N_TP, D).astype(jnp.float32)
        group_sums = jnp.einsum('ngf,gfd->ngd', hidden_groups, down_groups).astype(jnp.bfloat16)
        group_sums = lax.optimization_barrier(group_sums).astype(jnp.float32)
        return lax.optimization_barrier(jnp.sum(group_sums, axis=1)).astype(jnp.bfloat16)
    outputs = lax.map(run_expert, (buffer_rows, w_gate, w_up, w_down))
    picked = outputs[flat_ids, slot_ids].reshape(tok_total, TOP_K, D)
    combined = lax.optimization_barrier(jnp.sum(route_weights[:, :, None] * picked.astype(jnp.float32), axis=1))
    return combined.astype(jnp.bfloat16)

def reference(mix_tokens, mix_gain, w_query, w_key, w_value, query_gain, key_gain, w_out, expert_tokens, expert_gain, route_ids, route_weights, w_gate, w_up, w_down):
    mix_out = mixer_reference(mix_tokens, mix_gain, w_query, w_key, w_value, query_gain, key_gain, w_out)
    experts_out = experts_reference(expert_tokens, expert_gain, route_ids, route_weights, w_gate, w_up, w_down)
    return (mix_out, experts_out)
```

```python
import math

import jax
import jax.numpy as jnp
from jax import lax
from jax.sharding import PartitionSpec as P

HEAD = 64
GRID_W = 64


epsilon = 1e-06


def normalize(values, gain_vec):
    widened = values.astype(jnp.float32)
    return (
        widened
        * lax.rsqrt(jnp.mean(widened * widened, axis=-1, keepdims=True) + epsilon)
        * gain_vec
    )


def angle_tables(positions, head_size):
    quarter = head_size // 4
    frequency = 10000.0 ** (-jnp.arange(quarter, dtype=jnp.float32) / quarter)
    grid_pos = jnp.stack([positions // GRID_W, positions % GRID_W], axis=-1).astype(jnp.float32)
    angles = grid_pos[:, :, None] * frequency[None, None, :]
    return (jnp.cos(angles), jnp.sin(angles))


def turn(values, cosine_table, sine_table):
    shaped = values.shape
    quarter = shaped[-1] // 4
    leading = (shaped[0],) + (1,) * (len(shaped) - 2) + (2, quarter)
    cosine_table = cosine_table.reshape(leading)
    sine_table = sine_table.reshape(leading)
    halves = values.reshape(shaped[:-1] + (2, 2, quarter))
    first_part = halves[..., 0, :]
    second_part = halves[..., 1, :]
    turned = jnp.stack(
        [
            first_part * cosine_table - second_part * sine_table,
            first_part * sine_table + second_part * cosine_table,
        ],
        axis=-2,
    )
    return turned.reshape(shaped)


def attend(queries, fold_state, key_piece):
    key_rows = key_piece.shape[0]
    block_rows = math.gcd(key_rows, 1024)
    blocks = key_piece.reshape((key_rows // block_rows, block_rows) + key_piece.shape[1:])
    score_scale = HEAD ** (-0.5)

    def step_block(carried, block_keys):
        running_max, totals, accumulated = carried
        keys_part = block_keys[..., :HEAD]
        values_part = block_keys[..., HEAD:]
        scores = (
            jnp.einsum("qshd,ksd->qshk", queries, keys_part, preferred_element_type=jnp.float32)
            * score_scale
        )
        new_max = jnp.maximum(running_max, jnp.max(scores, axis=-1))
        shrink = jnp.exp(running_max - new_max)
        raised = jnp.exp(scores - new_max[..., None])
        totals = totals * shrink + jnp.sum(raised, axis=-1)
        accumulated = accumulated * shrink[..., None] + jnp.einsum(
            "qshk,ksd->qshd",
            raised.astype(jnp.bfloat16),
            values_part,
            preferred_element_type=jnp.float32,
        )
        return ((new_max, totals, accumulated), None)

    return lax.scan(step_block, fold_state, blocks)[0]


def mixer_half(mix_tokens, mix_gain, w_query, w_key, w_value, query_gain, key_gain, w_out):
    tp_count = lax.axis_size("tp")
    seq_rows, sequences, model_width = mix_tokens.shape
    head_count = w_query.shape[1] // HEAD
    key_heads = w_key.shape[1] // HEAD
    local_heads = head_count // tp_count
    normed = normalize(mix_tokens, mix_gain).astype(jnp.bfloat16)
    queries = jnp.dot(normed, w_query, preferred_element_type=jnp.float32).astype(jnp.bfloat16)
    keys_raw = jnp.dot(normed, w_key, preferred_element_type=jnp.float32).astype(jnp.bfloat16)
    values = jnp.dot(normed, w_value, preferred_element_type=jnp.float32).astype(jnp.bfloat16)
    queries = queries.reshape(seq_rows, sequences, tp_count, local_heads * HEAD)
    key_value = jnp.concatenate(
        [
            keys_raw.reshape(seq_rows, sequences, key_heads, HEAD),
            values.reshape(seq_rows, sequences, key_heads, HEAD),
        ],
        axis=-1,
    )
    key_value = jnp.repeat(key_value, tp_count // key_heads, axis=2)
    packed = jnp.concatenate([queries, key_value], axis=-1)
    arrived = lax.all_to_all(packed, "tp", split_axis=2, concat_axis=0, tiled=True)
    span_rows = arrived.shape[0]
    positions = lax.axis_index("ep") * span_rows + jnp.arange(span_rows, dtype=jnp.int32)
    cosine_table, sine_table = angle_tables(positions, HEAD)
    query_width = local_heads * HEAD
    own_queries = normalize(
        arrived[:, :, 0, :query_width].reshape(span_rows, sequences, local_heads, HEAD), query_gain
    )
    own_queries = turn(own_queries, cosine_table, sine_table).astype(jnp.bfloat16)
    own_keys = normalize(arrived[:, :, 0, query_width : query_width + HEAD], key_gain)
    own_keys = turn(own_keys, cosine_table, sine_table).astype(jnp.bfloat16)
    key_pairs = jnp.concatenate([own_keys, arrived[:, :, 0, query_width + HEAD :]], axis=-1)
    start_state = (
        jnp.full((span_rows, sequences, local_heads), -1e30, jnp.float32),
        jnp.zeros((span_rows, sequences, local_heads), jnp.float32),
        jnp.zeros((span_rows, sequences, local_heads, HEAD), jnp.float32),
    )
    running_max, totals, accumulated = attend(
        own_queries, start_state, lax.all_gather(key_pairs, "ep", axis=0, tiled=True)
    )
    mixed = (
        (accumulated / totals[..., None])
        .astype(jnp.bfloat16)
        .reshape(span_rows, sequences, query_width)
    )
    returned = lax.all_to_all(mixed, "tp", split_axis=0, concat_axis=2, tiled=True)
    return jnp.dot(returned, w_out, preferred_element_type=jnp.float32).astype(jnp.bfloat16)


def expert_sums(piece_rows, w_gate, w_up, w_down):
    gate_act = jnp.einsum("erd,edf->erf", piece_rows, w_gate, preferred_element_type=jnp.float32)
    up_act = jnp.einsum("erd,edf->erf", piece_rows, w_up, preferred_element_type=jnp.float32)
    hidden = (jax.nn.silu(gate_act) * up_act).astype(jnp.bfloat16)
    return jnp.einsum("erf,efd->erd", hidden, w_down, preferred_element_type=jnp.float32).astype(
        jnp.bfloat16
    )


def add_rounded(*terms):
    total = terms[0].astype(jnp.float32)
    for term in terms[1:]:
        total = total + term.astype(jnp.float32)
    return total.astype(jnp.bfloat16)


def chip_moves(chips, step):
    return [(2 * chip + core, 2 * (chip + step) + core) for chip in chips for core in range(2)]


def experts_on_line(rows, w_gate, w_up, w_down):
    tp_count = lax.axis_size("tp")
    chips = tp_count // 2
    place = lax.axis_index("tp") // 2
    partner = [(device, device ^ 1) for device in range(tp_count)]
    own_rows = rows.shape[1]
    from_right, from_left = [rows], [rows]
    for step in range(1, chips):
        from_right.append(
            lax.ppermute(from_right[-1], "tp", chip_moves(range(1, chips - step + 1), -1))
        )
        from_left.append(
            lax.ppermute(from_left[-1], "tp", chip_moves(range(step - 1, chips - 1), 1))
        )
    sums = [None] * chips
    order = [0] + sorted(range(1, chips), key=lambda slot: abs(2 * slot - chips))
    for slot in order:
        held = rows
        if slot:
            held = jnp.where(place + slot < chips, from_right[slot], from_left[chips - slot])
        both = jnp.concatenate([held, lax.ppermute(held, "tp", partner)], axis=1)
        group_sums = expert_sums(both, w_gate, w_up, w_down)
        given = lax.ppermute(group_sums[:, own_rows:], "tp", partner)
        sums[slot] = add_rounded(group_sums[:, :own_rows], given)
    rightward, leftward = None, None
    for step in range(1, chips):
        to_right = sums[chips - step]
        to_left = sums[step]
        if step > 1:
            to_right = add_rounded(to_right, rightward)
            to_left = add_rounded(to_left, leftward)
        rightward = lax.ppermute(to_right, "tp", chip_moves(range(step), 1))
        leftward = lax.ppermute(to_left, "tp", chip_moves(range(chips - step, chips), -1))
    if chips == 1:
        return sums[0]
    return add_rounded(sums[0], rightward, leftward)


def expert_half(expert_tokens, expert_gain, route_ids, route_weights, w_gate, w_up, w_down):
    ep_count = lax.axis_size("ep")
    tok_count, model_width = expert_tokens.shape
    top_count = route_ids.shape[1]
    local_experts = w_gate.shape[0]
    expert_count = local_experts * ep_count
    capacity = tok_count * top_count * 9 // (8 * expert_count)
    slot_count = expert_count * capacity
    normed = normalize(expert_tokens, expert_gain).astype(jnp.bfloat16)
    flat_ids = route_ids.reshape(-1)
    matches = (flat_ids[:, None] == jnp.arange(expert_count, dtype=jnp.int32)[None, :]).astype(
        jnp.int32
    )
    rank_ids = jnp.sum((jnp.cumsum(matches, axis=0) - 1) * matches, axis=1)
    slot_ids = flat_ids * capacity + rank_ids
    chosen = slot_ids.reshape(tok_count, top_count)
    dispatch = jnp.sum(
        (chosen[:, :, None] == jnp.arange(slot_count, dtype=jnp.int32)[None, None, :]).astype(
            jnp.bfloat16
        ),
        axis=1,
    )
    outgoing = lax.dot_general(
        dispatch, normed, (((0,), (0,)), ((), ())), preferred_element_type=jnp.float32
    )
    outgoing = outgoing.astype(jnp.bfloat16).reshape(ep_count, local_experts * capacity, model_width)
    incoming = lax.all_to_all(outgoing, "ep", split_axis=0, concat_axis=0, tiled=True)
    own_rows = ep_count * capacity
    incoming = incoming.reshape(ep_count, local_experts, capacity, model_width)
    incoming = incoming.transpose(1, 0, 2, 3).reshape(local_experts, own_rows, model_width)
    summed = experts_on_line(incoming, w_gate, w_up, w_down)
    expert_results = summed.reshape(local_experts, ep_count, capacity, model_width)
    expert_results = expert_results.transpose(1, 0, 2, 3).reshape(
        ep_count, local_experts * capacity, model_width
    )
    returned = lax.all_to_all(
        expert_results, "ep", split_axis=0, concat_axis=0, tiled=True
    ).reshape(slot_count, model_width)
    picked = jnp.take(returned, slot_ids, axis=0).reshape(tok_count, top_count, model_width)
    combined = jnp.sum(route_weights[:, :, None] * picked.astype(jnp.float32), axis=1)
    return combined.astype(jnp.bfloat16)


def body(
    mix_tokens,
    mix_gain,
    w_query,
    w_key,
    w_value,
    query_gain,
    key_gain,
    w_out,
    expert_tokens,
    expert_gain,
    route_ids,
    route_weights,
    w_gate,
    w_up,
    w_down,
):
    mix_out = mixer_half(mix_tokens, mix_gain, w_query, w_key, w_value, query_gain, key_gain, w_out)
    experts_out = expert_half(
        expert_tokens, expert_gain, route_ids, route_weights, w_gate, w_up, w_down
    )
    return (mix_out, experts_out)


def solution(mesh):
    placed = (
        P(("ep", "tp"), None, None),
        P(),
        P(),
        P(),
        P(),
        P(),
        P(),
        P(),
        P(("ep", "tp"), None),
        P(),
        P(("ep", "tp"), None),
        P(("ep", "tp"), None),
        P("ep", None, "tp"),
        P("ep", None, "tp"),
        P("ep", "tp", None),
    )
    return jax.shard_map(
        body,
        mesh=mesh,
        in_specs=placed,
        out_specs=(P(("ep", "tp"), None, None), P(("ep", "tp"), None)),
        check_vma=False,
    )
```

```python
import math

import jax
import jax.numpy as jnp
from jax import lax
from jax.experimental import pallas as pl
from jax.experimental.pallas import tpu as pltpu
from jax.sharding import PartitionSpec as P

HEAD = 64
GRID_W = 64


epsilon = 1e-06


def normalize(values, gain_vec):
    widened = values.astype(jnp.float32)
    return (
        widened
        * lax.rsqrt(jnp.mean(widened * widened, axis=-1, keepdims=True) + epsilon)
        * gain_vec
    )


def angle_tables(positions, head_size):
    quarter = head_size // 4
    frequency = 10000.0 ** (-jnp.arange(quarter, dtype=jnp.float32) / quarter)
    grid_pos = jnp.stack([positions // GRID_W, positions % GRID_W], axis=-1).astype(jnp.float32)
    angles = grid_pos[:, :, None] * frequency[None, None, :]
    return (jnp.cos(angles), jnp.sin(angles))


def turn(values, cosine_table, sine_table):
    shaped = values.shape
    quarter = shaped[-1] // 4
    leading = (shaped[0],) + (1,) * (len(shaped) - 2) + (2, quarter)
    cosine_table = cosine_table.reshape(leading)
    sine_table = sine_table.reshape(leading)
    halves = values.reshape(shaped[:-1] + (2, 2, quarter))
    first_part = halves[..., 0, :]
    second_part = halves[..., 1, :]
    turned = jnp.stack(
        [
            first_part * cosine_table - second_part * sine_table,
            first_part * sine_table + second_part * cosine_table,
        ],
        axis=-2,
    )
    return turned.reshape(shaped)


def attend(queries, fold_state, key_piece):
    key_rows = key_piece.shape[0]
    block_rows = math.gcd(key_rows, 1024)
    blocks = key_piece.reshape((key_rows // block_rows, block_rows) + key_piece.shape[1:])
    score_scale = HEAD ** (-0.5)

    def step_block(carried, block_keys):
        running_max, totals, accumulated = carried
        keys_part = block_keys[..., :HEAD]
        values_part = block_keys[..., HEAD:]
        scores = (
            jnp.einsum("qshd,ksd->qshk", queries, keys_part, preferred_element_type=jnp.float32)
            * score_scale
        )
        new_max = jnp.maximum(running_max, jnp.max(scores, axis=-1))
        shrink = jnp.exp(running_max - new_max)
        raised = jnp.exp(scores - new_max[..., None])
        totals = totals * shrink + jnp.sum(raised, axis=-1)
        accumulated = accumulated * shrink[..., None] + jnp.einsum(
            "qshk,ksd->qshd",
            raised.astype(jnp.bfloat16),
            values_part,
            preferred_element_type=jnp.float32,
        )
        return ((new_max, totals, accumulated), None)

    return lax.scan(step_block, fold_state, blocks)[0]


def mixer_front(mix_tokens, mix_gain, w_query, w_key, w_value, query_gain, key_gain):
    tp_count = lax.axis_size("tp")
    seq_rows, sequences, model_width = mix_tokens.shape
    head_count = w_query.shape[1] // HEAD
    key_heads = w_key.shape[1] // HEAD
    local_heads = head_count // tp_count
    normed = normalize(mix_tokens, mix_gain).astype(jnp.bfloat16)
    queries = jnp.dot(normed, w_query, preferred_element_type=jnp.float32).astype(jnp.bfloat16)
    keys_raw = jnp.dot(normed, w_key, preferred_element_type=jnp.float32).astype(jnp.bfloat16)
    values = jnp.dot(normed, w_value, preferred_element_type=jnp.float32).astype(jnp.bfloat16)
    queries = queries.reshape(seq_rows, sequences, tp_count, local_heads * HEAD)
    key_value = jnp.concatenate(
        [
            keys_raw.reshape(seq_rows, sequences, key_heads, HEAD),
            values.reshape(seq_rows, sequences, key_heads, HEAD),
        ],
        axis=-1,
    )
    key_value = jnp.repeat(key_value, tp_count // key_heads, axis=2)
    packed = jnp.concatenate([queries, key_value], axis=-1)
    arrived = lax.all_to_all(packed, "tp", split_axis=2, concat_axis=0, tiled=True)
    span_rows = arrived.shape[0]
    positions = lax.axis_index("ep") * span_rows + jnp.arange(span_rows, dtype=jnp.int32)
    cosine_table, sine_table = angle_tables(positions, HEAD)
    query_width = local_heads * HEAD
    own_queries = normalize(
        arrived[:, :, 0, :query_width].reshape(span_rows, sequences, local_heads, HEAD), query_gain
    )
    own_queries = turn(own_queries, cosine_table, sine_table).astype(jnp.bfloat16)
    own_keys = normalize(arrived[:, :, 0, query_width : query_width + HEAD], key_gain)
    own_keys = turn(own_keys, cosine_table, sine_table).astype(jnp.bfloat16)
    key_pairs = jnp.concatenate([own_keys, arrived[:, :, 0, query_width + HEAD :]], axis=-1)
    return own_queries, lax.all_gather(key_pairs, "ep", axis=0, tiled=True)


def mixer_back(own_queries, all_pairs, w_out):
    span_rows, sequences, local_heads, _ = own_queries.shape
    query_width = local_heads * HEAD
    start_state = (
        jnp.full((span_rows, sequences, local_heads), -1e30, jnp.float32),
        jnp.zeros((span_rows, sequences, local_heads), jnp.float32),
        jnp.zeros((span_rows, sequences, local_heads, HEAD), jnp.float32),
    )
    running_max, totals, accumulated = attend(
        own_queries, start_state, all_pairs
    )
    mixed = (
        (accumulated / totals[..., None])
        .astype(jnp.bfloat16)
        .reshape(span_rows, sequences, query_width)
    )
    returned = lax.all_to_all(mixed, "tp", split_axis=0, concat_axis=2, tiled=True)
    return jnp.dot(returned, w_out, preferred_element_type=jnp.float32).astype(jnp.bfloat16)


def expert_kernel(rows_ref, gate_ref, up_ref, down_ref, sums_ref):
    rows = rows_ref[0]
    gate_act = jnp.dot(rows, gate_ref[0], preferred_element_type=jnp.float32)
    up_act = jnp.dot(rows, up_ref[0], preferred_element_type=jnp.float32)
    hidden = (gate_act / (1.0 + jnp.exp(-gate_act)) * up_act).astype(jnp.bfloat16)
    sums_ref[0] = jnp.dot(hidden, down_ref[0], preferred_element_type=jnp.float32).astype(
        jnp.bfloat16
    )


def expert_sums(rows, w_gate, w_up, w_down):
    experts, row_count, model_width = rows.shape
    hidden_units = w_gate.shape[2]
    block_rows = math.gcd(row_count, 384)
    row_spec = pl.BlockSpec((1, block_rows, model_width), lambda e, r: (e, r, 0))
    in_spec = pl.BlockSpec((1, model_width, hidden_units), lambda e, r: (e, 0, 0))
    return pl.pallas_call(
        expert_kernel,
        grid=(experts, row_count // block_rows),
        in_specs=[
            row_spec,
            in_spec,
            in_spec,
            pl.BlockSpec((1, hidden_units, model_width), lambda e, r: (e, 0, 0)),
        ],
        out_specs=row_spec,
        out_shape=jax.ShapeDtypeStruct(rows.shape, jnp.bfloat16),
        compiler_params=pltpu.CompilerParams(vmem_limit_bytes=60 * 1024 * 1024),
        name="experts",
    )(rows, w_gate, w_up, w_down)


def route_rows(expert_tokens, expert_gain, route_ids, local_experts):
    ep_count = lax.axis_size("ep")
    tok_count, model_width = expert_tokens.shape
    top_count = route_ids.shape[1]
    expert_count = local_experts * ep_count
    capacity = tok_count * top_count * 9 // (8 * expert_count)
    slot_count = ep_count * capacity * local_experts
    normed = normalize(expert_tokens, expert_gain).astype(jnp.bfloat16)
    flat_ids = route_ids.reshape(-1)
    matches = (flat_ids[:, None] == jnp.arange(expert_count, dtype=jnp.int32)[None, :]).astype(
        jnp.int32
    )
    rank_ids = jnp.sum((jnp.cumsum(matches, axis=0) - 1) * matches, axis=1)
    slot_ids = (
        flat_ids // local_experts * capacity + rank_ids
    ) * local_experts + flat_ids % local_experts
    chosen = slot_ids.reshape(tok_count, top_count)
    dispatch = jnp.sum(
        (chosen[:, :, None] == jnp.arange(slot_count, dtype=jnp.int32)[None, None, :]).astype(
            jnp.bfloat16
        ),
        axis=1,
    )
    outgoing = lax.dot_general(
        dispatch, normed, (((0,), (0,)), ((), ())), preferred_element_type=jnp.float32
    )
    outgoing = outgoing.astype(jnp.bfloat16).reshape(ep_count, capacity, local_experts, model_width)
    incoming = lax.all_to_all(outgoing, "ep", split_axis=0, concat_axis=0, tiled=True)
    own_rows = ep_count * capacity
    incoming = incoming.reshape(own_rows, local_experts, model_width)
    return lax.all_gather(incoming, "tp", axis=0, tiled=True), slot_ids


def expert_half(all_rows, slot_ids, route_weights, capacity, w_gate, w_up, w_down):
    ep_count = lax.axis_size("ep")
    tok_count, top_count = route_weights.shape
    local_experts = w_gate.shape[0]
    model_width = all_rows.shape[-1]
    slot_count = ep_count * capacity * local_experts
    group_sums = expert_sums(all_rows.transpose(1, 0, 2), w_gate, w_up, w_down)
    summed = lax.psum_scatter(
        group_sums.transpose(1, 0, 2), "tp", scatter_dimension=0, tiled=True
    )
    expert_results = summed.reshape(ep_count, capacity, local_experts, model_width)
    returned = lax.all_to_all(
        expert_results, "ep", split_axis=0, concat_axis=0, tiled=True
    ).reshape(slot_count, model_width)
    picked = jnp.take(returned, slot_ids, axis=0).reshape(tok_count, top_count, model_width)
    combined = jnp.sum(route_weights[:, :, None] * picked.astype(jnp.float32), axis=1)
    return combined.astype(jnp.bfloat16)


def body(
    mix_tokens,
    mix_gain,
    w_query,
    w_key,
    w_value,
    query_gain,
    key_gain,
    w_out,
    expert_tokens,
    expert_gain,
    route_ids,
    route_weights,
    w_gate,
    w_up,
    w_down,
):
    tok_count, top_count = route_ids.shape
    local_experts = w_gate.shape[0]
    capacity = tok_count * top_count * 9 // (8 * local_experts * lax.axis_size("ep"))
    all_rows, slot_ids = route_rows(expert_tokens, expert_gain, route_ids, local_experts)
    own_queries, all_pairs = mixer_front(
        mix_tokens, mix_gain, w_query, w_key, w_value, query_gain, key_gain
    )
    all_rows, all_pairs = lax.optimization_barrier((all_rows, all_pairs))
    experts_out = expert_half(all_rows, slot_ids, route_weights, capacity, w_gate, w_up, w_down)
    mix_out = mixer_back(own_queries, all_pairs, w_out)
    return (mix_out, experts_out)


def solution(mesh):
    placed = (
        P(("ep", "tp"), None, None),
        P(),
        P(),
        P(),
        P(),
        P(),
        P(),
        P(),
        P(("ep", "tp"), None),
        P(),
        P(("ep", "tp"), None),
        P(("ep", "tp"), None),
        P("ep", None, "tp"),
        P("ep", None, "tp"),
        P("ep", "tp", None),
    )
    return jax.shard_map(
        body,
        mesh=mesh,
        in_specs=placed,
        out_specs=(P(("ep", "tp"), None, None), P(("ep", "tp"), None)),
        check_vma=False,
    )
```
